512 devices in a mesh: ep: 16 (over y, x), tp: 32 (over z, core).
Axes of the slice: x: 4, y: 4, z: 16, core: 2. Of those that a mesh axis runs over, the one named last changes fastest.
Arguments:
- tokens: bfloat16 [512, 2048], P('ep'), may hold values from -6 to 6
- norm_gain: float32 [2048], replicated, may hold values from 0.1 to 1.9
- routes: int32 [512, 2], P('ep'), may hold values from 0 to 15, all different within a row; in each aligned block of 32 rows (0 to 31, 32 to 63, ...) at most 16 rows name the same one
- gate_weights: float32 [512, 2], P('ep'), may hold values from 0.1 to 1
- expert_gate: bfloat16 [16, 2048, 8192], P('ep', None, 'tp'), may hold values from -0.125 to 0.125
- expert_up: bfloat16 [16, 2048, 8192], P('ep', None, 'tp'), may hold values from -0.125 to 0.125
- expert_down: bfloat16 [16, 8192, 2048], P('ep', 'tp'), may hold values from -0.0625 to 0.0625
Outputs:
- mixed: bfloat16 [512, 2048], P('ep', 'tp')
The draws below stay inside these ranges and needn't reach their ends.
Inputs may be any that keep to these rules, and one draw needn't show every extreme that they name: `routes`: each row names 2 different experts; among the rows of one index of ep no expert is named by more than 16 rows.
All inputs are finite; a program needn't handle non-finite values.
Results may differ from the reference program's by a relative error of at most 0.0095.
Values may be sent and summed in bfloat16 or wider, within the bound.
No kernel may reach another device: no remote copies, remote signals or barrier semaphores. Data moves between devices by JAX's collectives and lax.ppermute only.
A program may use at most 64 MiB of HBM per device.

```python
import math
import jax
import jax.numpy as jnp
import numpy as np
from jax import lax

D = 2048
FF = 8192
TOP = 2
TOK_DEV = 32
EXPERTS = 16
CAP = 16
TOKENS = 512


def shard_levels(rng, shape, pieces, low, high):
    def one(position, blocks):
        steps = jax.random.uniform(jax.random.fold_in(jax.random.fold_in(rng, 6), position), (blocks,), jnp.float32, low / len(pieces), high / len(pieces))
        return jnp.repeat(jnp.exp(steps), shape[position] // blocks).reshape((-1,) + (1,) * (len(shape) - position - 1))

    gain = one(*pieces[0])
    for cut in pieces[1:]:
        gain = gain * one(*cut)
    return gain


def routed_block(key, own, number, rows, count, top, limit, slope):
    order = jax.random.permutation(key, count)
    heavy_load, common = portions_of(count, rows * top, limit, slope, True), portions_of(count, rows * top, limit, slope, False)
    places = jnp.arange(count)

    def named(tallies, offset_by):
        used = int((tallies > 0).sum())
        fixed = max(1, used // 4)
        shifted = fixed + (places - fixed + offset_by * (used - fixed)) % max(1, count - fixed)
        return jnp.zeros((count,), jnp.int32).at[order[jnp.where(places < fixed, places, shifted)]].set(jnp.asarray(tallies, jnp.int32))

    tallies = jnp.where(number % 4 == 0, named(heavy_load, number // 4), named(common, number - number // 4 - 1))
    mixed = jax.random.permutation(jax.random.fold_in(own, 3), count)
    giver, taker = mixed[0:count // 2 * 2:2], mixed[1:count // 2 * 2:2]
    room = jnp.minimum(tallies[giver] - 1, limit - tallies[taker]) // 2
    room = jnp.where((giver == order[0]) | (taker == order[0]) | (tallies[taker] == 0), 0, jnp.maximum(room, 0))
    shifted = jax.random.randint(jax.random.fold_in(own, 4), (count // 2,), 0, 1 << 20) % (room + 1)
    tallies = tallies.at[giver].add(-shifted).at[taker].add(shifted)
    members = jnp.searchsorted(jnp.cumsum(tallies), jnp.arange(rows * top), side="right").astype(jnp.int32)
    table = members.reshape(top, rows).T
    table = table[jax.random.permutation(jax.random.fold_in(own, 1), rows)]
    offset_by = jax.random.randint(jax.random.fold_in(own, 2), (rows, 1), 0, top)
    return jnp.take_along_axis(table, (jnp.arange(top)[None, :] + offset_by) % top, axis=1)


def portions_of(number_of, total, most, lean, full):
    weights = [(1 << 20) // math.isqrt(grade ** lean) + 1 for grade in range(1, number_of + 1)]
    largest = most if full else min(most, max(-(-total // number_of), total * weights[0] // sum(weights)))
    least = 1 if total - largest >= number_of - 1 else 0
    holding, spare = [largest] + [least] * (number_of - 1), total - largest - least * (number_of - 1)
    while spare > 0:
        free = [i for i in range(1, number_of) if holding[i] < largest] or [i for i in range(1, number_of) if holding[i] < most]
        mass, left = sum([weights[i] for i in free]), spare
        for i in free:
            extra = min(most - holding[i], max(1, left * weights[i] // mass), spare)
            holding[i] = holding[i] + extra
            spare = spare - extra
    return np.array(holding)


def noise(key, shape, width, most, shards=(), kind=jnp.bfloat16):
    entries = jax.random.normal(key, shape, jnp.float32) * width
    if len(shards) > 0:
        entries = shard_levels(key, shape, shards, -0.22, 0.18) * entries
    return jnp.clip(entries, min=-most, max=most).astype(kind)


def setup_inputs(seed: int = 0) -> dict:
    key_list = jax.random.split(jax.random.key(seed), 8)
    tokens = noise(key_list[0], (TOKENS, D), 1.0, 6.0, ((0, 16),))
    norm_gain = jnp.clip(1.0 + 0.18 * jax.random.normal(key_list[1], (D,), jnp.float32), 0.1, 1.9)
    routes_keys = jax.random.split(jax.random.fold_in(key_list[2], 1), TOKENS // TOK_DEV)
    routes_turns = jax.random.permutation(jax.random.fold_in(key_list[2], 3), TOKENS // TOK_DEV)
    routes = jax.vmap(lambda own, number: routed_block(jax.random.fold_in(key_list[2], 2), own, number, TOK_DEV, EXPERTS, TOP, CAP, 2))(routes_keys, routes_turns).reshape((TOKENS, TOP))
    gate_weights = jnp.clip(0.1 + 0.9 * jax.random.uniform(key_list[3], (TOKENS, TOP), jnp.float32) ** shard_levels(key_list[3], (TOKENS, TOP), ((0, 16),), -0.2, 0.2), 0.1, 1.0)
    expert_gate = noise(key_list[4], (EXPERTS, D, FF), D ** -0.5, 0.125, ((0, 16), (2, 32)))
    expert_up = noise(key_list[5], (EXPERTS, D, FF), D ** -0.5, 0.125, ((0, 16), (2, 32)))
    expert_down = noise(key_list[6], (EXPERTS, FF, D), FF ** -0.5, 0.0625, ((0, 16), (1, 32)))
    return {"tokens": tokens, "norm_gain": norm_gain, "routes": routes, "gate_weights": gate_weights, "expert_gate": expert_gate, "expert_up": expert_up, "expert_down": expert_down}


def reference(tokens, norm_gain, routes, gate_weights, expert_gate, expert_up, expert_down):
    values = tokens.astype(jnp.float32)
    scale = lax.rsqrt(lax.optimization_barrier(jnp.mean(values * values, axis=-1, keepdims=True)) + 1e-06)
    normed = (values * scale * norm_gain[None, :]).astype(jnp.bfloat16)
    chosen = (routes[:, :, None] == jnp.arange(EXPERTS, dtype=jnp.int32)[None, None, :]).astype(jnp.float32)
    coefs = lax.optimization_barrier(jnp.sum(gate_weights[:, :, None] * chosen, axis=1))

    def expert_step(total, packed):
        w_gate, w_up, w_down, weight = packed
        gate = jnp.dot(normed, w_gate, preferred_element_type=jnp.float32)
        upper = jnp.dot(normed, w_up, preferred_element_type=jnp.float32)
        hidden = (jax.nn.silu(gate) * upper).astype(jnp.bfloat16)
        output = jnp.dot(hidden, w_down, preferred_element_type=jnp.float32)
        return (total + weight[:, None] * output, None)
    start = jnp.zeros((tokens.shape[0], tokens.shape[1]), jnp.float32)
    total, _ = lax.scan(expert_step, start, (expert_gate, expert_up, expert_down, coefs.T))
    return total.astype(jnp.bfloat16)
```

```python
import jax
import jax.numpy as jnp
import numpy as np
from jax import lax
from jax.experimental import pallas as pl
from jax.experimental.pallas import tpu as pltpu
from jax.sharding import Mesh
from jax.sharding import PartitionSpec as P

LANES = 128
HALF = LANES // 2
F32 = jnp.float32
BF16 = jnp.bfloat16
SWAP = ((0, 1), (1, 0))


def params(mib):
    return pltpu.CompilerParams(vmem_limit_bytes=mib * 2**20)


def flipped(x):
    return pltpu.roll(x, HALF, axis=x.ndim - 1)


def column(row, eye):
    return jnp.sum(jnp.where(eye, row, 0), axis=1, keepdims=True)


def dispatch_kernel(tok_ref, gain_ref, picks_ref, weight_ref, buffer_ref, combine_ref):
    rows, width = tok_ref.shape
    slots = buffer_ref.shape[0]
    cap = rows // 2
    part = width // 2
    first = pl.multiple_of(lax.axis_index("c") * part, part)
    values = tok_ref[...].astype(F32)
    scale = lax.rsqrt(jnp.mean(values * values, axis=-1, keepdims=True) + 1e-06)
    mine = tok_ref[:, pl.ds(first, part)].astype(F32)
    normed = (mine * scale * gain_ref[:, pl.ds(first, part)]).astype(BF16)

    at_row = lax.broadcasted_iota(jnp.int32, (rows, rows), 0)
    at_col = lax.broadcasted_iota(jnp.int32, (rows, rows), 1)
    eye = at_row == at_col
    earlier = (at_col < at_row).astype(F32).astype(BF16)
    pick0 = column(picks_ref[0:1, :], eye)
    pick1 = column(picks_ref[1:2, :], eye)
    weight0 = column(weight_ref[0:1, :], eye)
    weight1 = column(weight_ref[1:2, :], eye)
    slot = lax.broadcasted_iota(jnp.int32, (rows, slots), 1)
    expert = slot // cap
    place = (slot % cap).astype(F32)
    is0 = pick0 == expert
    is1 = pick1 == expert
    chosen = (is0 | is1).astype(F32)
    rank = jnp.dot(earlier, chosen.astype(BF16), preferred_element_type=F32)
    table = jnp.where(rank == place, chosen, 0.0)
    buffer_ref[...] = jnp.dot(
        table.T.astype(BF16), normed, preferred_element_type=F32
    ).astype(BF16)
    weights = table * jnp.where(is0, weight0, weight1)
    high = weights.astype(BF16)
    combine_ref[0:rows, :] = high
    combine_ref[rows:, :] = (weights - high.astype(F32)).astype(BF16)


def first_half_kernel(rows_ref, gate_ref, up_ref, gate_out, up_out):
    part = rows_ref.shape[1]
    first = pl.multiple_of(lax.axis_index("c") * part, part)
    rows = rows_ref[...]
    gate_out[...] = jnp.dot(rows, gate_ref[pl.ds(first, part), :], preferred_element_type=F32)
    up_out[...] = jnp.dot(rows, up_ref[pl.ds(first, part), :], preferred_element_type=F32)


def expert_kernel(rows_ref, gate_in, up_in, gate_ref, up_ref, down_ref, mine_out, send_out):
    part = rows_ref.shape[1]
    core = lax.axis_index("c")
    first = pl.multiple_of((1 - core) * part, part)
    rows = rows_ref[...]
    gate = gate_in[...] + jnp.dot(
        rows, gate_ref[pl.ds(first, part), :], preferred_element_type=F32
    )
    upper = up_in[...] + jnp.dot(rows, up_ref[pl.ds(first, part), :], preferred_element_type=F32)
    hidden = (gate / (1.0 + jnp.exp(-gate)) * upper).astype(BF16)
    is_low = core == 0
    lane = lax.broadcasted_iota(jnp.int32, (rows.shape[0], LANES), 1)
    low_lane = lane < HALF
    stay = low_lane == is_low
    for m in range(mine_out.shape[1] // LANES):
        pair = jnp.dot(
            hidden, down_ref[:, 2 * m * LANES : 2 * (m + 1) * LANES], preferred_element_type=F32
        )
        a, b = pair[:, :LANES], pair[:, LANES:]
        at = slice(m * LANES, (m + 1) * LANES)
        keep, move = jnp.where(is_low, a, b), jnp.where(is_low, b, a)
        mine_out[:, at] = jnp.where(stay, keep, flipped(move))
        send_out[:, at] = jnp.where(stay, flipped(keep), move).astype(BF16)


def combine_kernel(table_ref, back_ref, out_ref):
    rows = table_ref.shape[0] // 2
    half = rows // 2
    both = jnp.dot(table_ref[...], back_ref[...], preferred_element_type=F32)
    mixed = both[:rows] + both[rows:]
    low_lane = lax.broadcasted_iota(jnp.int32, (half, LANES), 1) < HALF
    for m in range(back_ref.shape[1] // LANES):
        at = slice(m * LANES, (m + 1) * LANES)
        a, b = mixed[:half, at], mixed[half:, at]
        out_ref[2 * m] = jnp.where(low_lane, a, flipped(b)).astype(BF16)
        out_ref[2 * m + 1] = jnp.where(low_lane, flipped(a), b).astype(BF16)


def total_kernel(parts_ref, out_ref):
    half = out_ref.shape[0] // 2
    total = jnp.sum(parts_ref[...].astype(F32), axis=0)
    out_ref[:half, :] = total[:, :HALF].astype(BF16)
    out_ref[half:, :] = flipped(total)[:, :HALF].astype(BF16)


def shape(dims, dtype):
    return jax.ShapeDtypeStruct(dims, dtype)


def shards(tokens, norm_gain, routes, gate_weights, expert_gate, expert_up, expert_down):
    rows, width = tokens.shape
    n_ep = lax.axis_size("ep")
    n_z = lax.axis_size("z")
    cap = rows // 2
    slots = n_ep * cap
    part = width // 2
    w_gate, w_up, w_down = expert_gate[0], expert_up[0], expert_down[0]
    units = w_gate.shape[1]

    buffer, table = pl.pallas_call(
        dispatch_kernel,
        out_shape=(shape((slots, part), BF16), shape((2 * rows, slots), BF16)),
        compiler_params=params(8),
        name="dispatch",
    )(tokens, norm_gain[None, :], routes.T, gate_weights.T)
    received = lax.all_to_all(
        buffer.reshape(n_ep, cap, part), "ep", split_axis=0, concat_axis=0, tiled=True
    ).reshape(slots, part)
    other = lax.ppermute(received, "c", SWAP)
    gate, upper = pl.pallas_call(
        first_half_kernel,
        out_shape=(shape((slots, units), F32), shape((slots, units), F32)),
        compiler_params=params(8),
        name="first_half",
    )(received, w_gate, w_up)
    mine, send = pl.pallas_call(
        expert_kernel,
        out_shape=(shape((slots, part), F32), shape((slots, part), BF16)),
        compiler_params=params(12),
        name="expert",
    )(other, gate, upper, w_gate, w_up, w_down)
    arrived = lax.ppermute(send, "c", SWAP)
    outputs = (mine + arrived.astype(F32)).astype(BF16)
    back = lax.all_to_all(
        outputs.reshape(n_ep, cap, part), "ep", split_axis=0, concat_axis=0, tiled=True
    ).reshape(slots, part)
    packed = pl.pallas_call(
        combine_kernel,
        out_shape=shape((n_z, rows // 2, LANES), BF16),
        compiler_params=params(8),
        name="combine",
    )(table, back)
    parts = lax.all_to_all(packed, "z", split_axis=0, concat_axis=0, tiled=True)
    return pl.pallas_call(
        total_kernel,
        out_shape=shape((rows, HALF), BF16),
        compiler_params=params(8),
        name="total",
    )(parts)


def solution(mesh):
    n_ep, n_tp = mesh.devices.shape
    chips = Mesh(np.asarray(mesh.devices).reshape(n_ep, n_tp // 2, 2), ("ep", "z", "c"))
    tp = ("z", "c")
    placed = (
        P("ep", None),
        P(),
        P("ep", None),
        P("ep", None),
        P("ep", None, tp),
        P("ep", None, tp),
        P("ep", tp, None),
    )
    return jax.shard_map(
        shards, mesh=chips, in_specs=placed, out_specs=P("ep", tp), check_vma=False
    )
```

```python
import jax
import jax.numpy as jnp
import numpy as np
from jax import lax
from jax.experimental import pallas as pl
from jax.experimental.pallas import tpu as pltpu
from jax.sharding import Mesh
from jax.sharding import PartitionSpec as P

LANES = 128
HALF = LANES // 2
F32 = jnp.float32
BF16 = jnp.bfloat16
SWAP = ((0, 1), (1, 0))


def params(mib):
    return pltpu.CompilerParams(vmem_limit_bytes=mib * 2**20)


def flipped(x):
    return pltpu.roll(x, HALF, axis=x.ndim - 1)


def column(row, eye):
    return jnp.sum(jnp.where(eye, row, 0), axis=1, keepdims=True)


def in_hbm(*arrays):
    return [pltpu.with_memory_space_constraint(x, pltpu.HBM) for x in arrays]


def started(sems, *pairs):
    copies = [pltpu.make_async_copy(src, dst, sems.at[i]) for i, (src, dst) in enumerate(pairs)]
    for copy in copies:
        copy.start()
    return copies


def dispatch_kernel(
    tok_hbm,
    gain_hbm,
    picks_hbm,
    weight_hbm,
    gate_hbm,
    up_hbm,
    down_hbm,
    buffer_ref,
    combine_ref,
    gate_ref,
    up_ref,
    down_ref,
    tok,
    gain,
    picks,
    weight,
    sems,
):
    rows, width = tok.shape
    slots = buffer_ref.shape[0]
    cap = rows // 2
    part = width // 2
    core = lax.axis_index("c")
    first = pl.multiple_of(core * part, part)
    second = pl.multiple_of((1 - core) * part, part)
    copies = started(
        sems,
        (picks_hbm, picks),
        (weight_hbm, weight),
        (tok_hbm, tok),
        (gain_hbm, gain),
        (gate_hbm.at[pl.ds(second, part), :], gate_ref),
        (up_hbm.at[pl.ds(second, part), :], up_ref),
        (down_hbm, down_ref),
    )

    at_row = lax.broadcasted_iota(jnp.int32, (rows, rows), 0)
    at_col = lax.broadcasted_iota(jnp.int32, (rows, rows), 1)
    eye = at_row == at_col
    earlier = (at_col < at_row).astype(F32).astype(BF16)
    slot = lax.broadcasted_iota(jnp.int32, (rows, slots), 1)
    expert = slot // cap
    place = (slot % cap).astype(F32)
    copies[0].wait()
    copies[1].wait()
    pick0 = column(picks[0:1, :], eye)
    pick1 = column(picks[1:2, :], eye)
    weight0 = column(weight[0:1, :], eye)
    weight1 = column(weight[1:2, :], eye)
    is0 = pick0 == expert
    is1 = pick1 == expert
    chosen = (is0 | is1).astype(F32)
    rank = jnp.dot(earlier, chosen.astype(BF16), preferred_element_type=F32)
    table = jnp.where(rank == place, chosen, 0.0)
    weights = table * jnp.where(is0, weight0, weight1)
    high = weights.astype(BF16)
    combine_ref[0:rows, :] = high
    combine_ref[rows:, :] = (weights - high.astype(F32)).astype(BF16)
    spread = table.T.astype(BF16)

    copies[2].wait()
    copies[3].wait()
    values = tok[...].astype(F32)
    scale = lax.rsqrt(jnp.mean(values * values, axis=-1, keepdims=True) + 1e-06)
    mine = tok[:, pl.ds(first, part)].astype(F32)
    normed = (mine * scale * gain[:, pl.ds(first, part)]).astype(BF16)
    buffer_ref[...] = jnp.dot(spread, normed, preferred_element_type=F32).astype(BF16)
    for copy in copies[4:]:
        copy.wait()


def first_half_kernel(rows_ref, gate_hbm, up_hbm, gate_out, up_out, gate, up, sems):
    part = rows_ref.shape[1]
    first = pl.multiple_of(lax.axis_index("c") * part, part)
    copies = started(
        sems, (gate_hbm.at[pl.ds(first, part), :], gate), (up_hbm.at[pl.ds(first, part), :], up)
    )
    rows = rows_ref[...]
    copies[0].wait()
    gate_out[...] = jnp.dot(rows, gate[...], preferred_element_type=F32)
    copies[1].wait()
    up_out[...] = jnp.dot(rows, up[...], preferred_element_type=F32)


def expert_kernel(rows_ref, gate_in, up_in, gate_ref, up_ref, down_ref, mine_out, send_out):
    rows = rows_ref[...]
    gate = gate_in[...] + jnp.dot(rows, gate_ref[...], preferred_element_type=F32)
    upper = up_in[...] + jnp.dot(rows, up_ref[...], preferred_element_type=F32)
    hidden = (gate / (1.0 + jnp.exp(-gate)) * upper).astype(BF16)
    is_low = lax.axis_index("c") == 0
    lane = lax.broadcasted_iota(jnp.int32, (rows.shape[0], LANES), 1)
    stay = (lane < HALF) == is_low
    for m in range(mine_out.shape[1] // LANES):
        pair = jnp.dot(
            hidden, down_ref[:, 2 * m * LANES : 2 * (m + 1) * LANES], preferred_element_type=F32
        )
        a, b = pair[:, :LANES], pair[:, LANES:]
        at = slice(m * LANES, (m + 1) * LANES)
        keep, move = jnp.where(is_low, a, b), jnp.where(is_low, b, a)
        mine_out[:, at] = jnp.where(stay, keep, flipped(move))
        send_out[:, at] = jnp.where(stay, flipped(keep), move).astype(BF16)


def combine_kernel(table_ref, back_ref, out_ref):
    rows = table_ref.shape[0] // 2
    half = rows // 2
    both = jnp.dot(table_ref[...], back_ref[...], preferred_element_type=F32)
    mixed = both[:rows] + both[rows:]
    low_lane = lax.broadcasted_iota(jnp.int32, (half, LANES), 1) < HALF
    for m in range(back_ref.shape[1] // LANES):
        at = slice(m * LANES, (m + 1) * LANES)
        a, b = mixed[:half, at], mixed[half:, at]
        out_ref[2 * m] = jnp.where(low_lane, a, flipped(b)).astype(BF16)
        out_ref[2 * m + 1] = jnp.where(low_lane, flipped(a), b).astype(BF16)


def total_kernel(parts_ref, out_ref):
    half = out_ref.shape[0] // 2
    total = jnp.sum(parts_ref[...].astype(F32), axis=0)
    out_ref[:half, :] = total[:, :HALF].astype(BF16)
    out_ref[half:, :] = flipped(total)[:, :HALF].astype(BF16)


def shape(dims, dtype):
    return jax.ShapeDtypeStruct(dims, dtype)


def shards(tokens, norm_gain, routes, gate_weights, expert_gate, expert_up, expert_down):
    rows, width = tokens.shape
    n_ep = lax.axis_size("ep")
    n_z = lax.axis_size("z")
    cap = rows // 2
    slots = n_ep * cap
    part = width // 2
    w_gate, w_up, w_down = expert_gate[0], expert_up[0], expert_down[0]
    units = w_gate.shape[1]

    gain = norm_gain[None, :]
    picks = routes.T
    weights = gate_weights.T
    hbm = pl.BlockSpec(memory_space=pltpu.HBM)
    vmem = pl.BlockSpec(memory_space=pltpu.VMEM)
    buffer, table, gate_rest, up_rest, down = pl.pallas_call(
        dispatch_kernel,
        in_specs=[hbm] * 7,
        out_shape=(
            shape((slots, part), BF16),
            shape((2 * rows, slots), BF16),
            shape((part, units), BF16),
            shape((part, units), BF16),
            shape(w_down.shape, BF16),
        ),
        scratch_shapes=[
            pltpu.VMEM(tokens.shape, tokens.dtype),
            pltpu.VMEM(gain.shape, gain.dtype),
            pltpu.VMEM(picks.shape, picks.dtype),
            pltpu.VMEM(weights.shape, weights.dtype),
            pltpu.SemaphoreType.DMA((7,)),
        ],
        compiler_params=params(8),
        name="dispatch",
    )(*in_hbm(tokens, gain, picks, weights, w_gate, w_up, w_down))
    received = lax.all_to_all(
        buffer.reshape(n_ep, cap, part), "ep", split_axis=0, concat_axis=0, tiled=True
    ).reshape(slots, part)
    other = lax.ppermute(received, "c", SWAP)
    gate, upper = pl.pallas_call(
        first_half_kernel,
        in_specs=[vmem, hbm, hbm],
        out_shape=(shape((slots, units), F32), shape((slots, units), F32)),
        scratch_shapes=[
            pltpu.VMEM((part, units), BF16),
            pltpu.VMEM((part, units), BF16),
            pltpu.SemaphoreType.DMA((2,)),
        ],
        compiler_params=params(8),
        name="first_half",
    )(received, *in_hbm(w_gate, w_up))
    mine, send = pl.pallas_call(
        expert_kernel,
        out_shape=(shape((slots, part), F32), shape((slots, part), BF16)),
        compiler_params=params(12),
        name="expert",
    )(other, gate, upper, gate_rest, up_rest, down)
    arrived = lax.ppermute(send, "c", SWAP)
    outputs = (mine + arrived.astype(F32)).astype(BF16)
    back = lax.all_to_all(
        outputs.reshape(n_ep, cap, part), "ep", split_axis=0, concat_axis=0, tiled=True
    ).reshape(slots, part)
    packed = pl.pallas_call(
        combine_kernel,
        out_shape=shape((n_z, rows // 2, LANES), BF16),
        compiler_params=params(8),
        name="combine",
    )(table, back)
    parts = lax.all_to_all(packed, "z", split_axis=0, concat_axis=0, tiled=True)
    return pl.pallas_call(
        total_kernel,
        out_shape=shape((rows, HALF), BF16),
        compiler_params=params(8),
        name="total",
    )(parts)


def solution(mesh):
    n_ep, n_tp = mesh.devices.shape
    chips = Mesh(np.asarray(mesh.devices).reshape(n_ep, n_tp // 2, 2), ("ep", "z", "c"))
    tp = ("z", "c")
    placed = (
        P("ep", None),
        P(),
        P("ep", None),
        P("ep", None),
        P("ep", None, tp),
        P("ep", None, tp),
        P("ep", tp, None),
    )
    return jax.shard_map(
        shards, mesh=chips, in_specs=placed, out_specs=P("ep", tp), check_vma=False
    )
```

```python
import jax
import jax.numpy as jnp
import numpy as np
from jax import lax
from jax.experimental import pallas as pl
from jax.experimental.pallas import tpu as pltpu
from jax.sharding import Mesh
from jax.sharding import PartitionSpec as P


LANES = 128
HALF = LANES // 2
F32 = jnp.float32
BF16 = jnp.bfloat16
SWAP = ((0, 1), (1, 0))


def params(mib):
    return pltpu.CompilerParams(vmem_limit_bytes=mib * 2**20)


def flipped(x):
    return pltpu.roll(x, HALF, axis=x.ndim - 1)


def column(row, eye):
    return jnp.sum(jnp.where(eye, row, 0), axis=1, keepdims=True)


def in_hbm(*arrays):
    return [pltpu.with_memory_space_constraint(x, pltpu.HBM) for x in arrays]


def started(sems, *pairs):
    copies = [pltpu.make_async_copy(src, dst, sems.at[i]) for i, (src, dst) in enumerate(pairs)]
    for copy in copies:
        copy.start()
    return copies


def dispatch_kernel(
    tok_hbm,
    gain_hbm,
    picks_hbm,
    weight_hbm,
    buffer_hbm,
    combine_ref,
    tok,
    gain,
    picks,
    weight,
    buffer,
    sems,
    out_sems,
):
    copies = started(
        sems, (tok_hbm, tok), (gain_hbm, gain), (picks_hbm, picks), (weight_hbm, weight)
    )
    rows, width = tok.shape
    slots = combine_ref.shape[1]
    cap = rows // 2
    core = lax.axis_index("c")

    at_row = lax.broadcasted_iota(jnp.int32, (rows, rows), 0)
    at_col = lax.broadcasted_iota(jnp.int32, (rows, rows), 1)
    eye = at_row == at_col
    earlier = (at_col < at_row).astype(F32).astype(BF16)
    copies[2].wait()
    copies[3].wait()
    pick0 = column(picks[0:1, :], eye)
    pick1 = column(picks[1:2, :], eye)
    weight0 = column(weight[0:1, :], eye)
    weight1 = column(weight[1:2, :], eye)

    def placed(count, each, base):
        slot = lax.broadcasted_iota(jnp.int32, (rows, count), 1)
        expert = slot // each
        is0 = pick0 == expert
        chosen = (is0 | (pick1 == expert)).astype(F32)
        rank = jnp.dot(earlier, chosen.astype(BF16), preferred_element_type=F32)
        place = (slot % each + base).astype(F32)
        return jnp.where(rank == place, chosen, 0.0), is0

    mine, _ = placed(slots // 2, cap // 2, core * (cap // 2))
    spread = mine.T.astype(BF16)
    table, is0 = placed(slots, cap, 0)
    weights = table * jnp.where(is0, weight0, weight1)
    high = weights.astype(BF16)
    combine_ref[0:rows, :] = high
    combine_ref[rows:, :] = (weights - high.astype(F32)).astype(BF16)

    copies[0].wait()
    copies[1].wait()
    values = tok[...].astype(F32)
    scale = lax.rsqrt(jnp.mean(values * values, axis=-1, keepdims=True) + 1e-06)
    chunks = out_sems.shape[0]
    leaving = []
    for i in range(chunks):
        at = pl.ds(i * (width // chunks), width // chunks)
        normed = (tok[:, at].astype(F32) * scale * gain[:, at]).astype(BF16)
        buffer[:, at] = jnp.dot(spread, normed, preferred_element_type=F32).astype(BF16)
        leaving.append(
            pltpu.make_async_copy(buffer.at[:, at], buffer_hbm.at[:, at], out_sems.at[i])
        )
        leaving[-1].start()
    for copy in leaving:
        copy.wait()


def load_kernel(src_hbm, dst, sems):
    (copy,) = started(sems, (src_hbm.at[pl.ds(0, dst.shape[0]), :], dst))
    copy.wait()


def times(a, w):
    return jnp.dot(a, w[...], preferred_element_type=F32)


def hidden_of(gate, upper):
    return (gate / (1.0 + jnp.exp(-gate)) * upper).astype(BF16)


def hidden_kernel(
    rows_ref,
    head0,
    gate0_hbm,
    up0_hbm,
    gate1_hbm,
    down0_hbm,
    hidden0_ref,
    gate1_out,
    down0_ref,
    tail0,
    up0,
    gate1,
    sems,
):
    cut = head0.shape[0]
    copies = started(
        sems,
        (gate0_hbm.at[pl.ds(cut, tail0.shape[0]), :], tail0),
        (up0_hbm, up0),
        (gate1_hbm, gate1),
        (down0_hbm, down0_ref),
    )
    gate = times(rows_ref[:, :cut], head0)
    copies[0].wait()
    gate = gate + times(rows_ref[:, cut:], tail0)
    copies[1].wait()
    hidden0_ref[...] = hidden_of(gate, times(rows_ref[...], up0))
    copies[2].wait()
    gate1_out[...] = times(rows_ref[...], gate1)
    copies[3].wait()


def down_kernel(rows_ref, up1, gate1_in, hidden0_ref, down0_ref, down1_ref, out_ref):
    n_ep, _, cap, part = out_ref.shape
    hidden0 = hidden0_ref[...]
    hidden1 = hidden_of(gate1_in[...], times(rows_ref[...], up1))
    low_lane = lax.broadcasted_iota(jnp.int32, (n_ep * cap, LANES), 1) < HALF
    for m in range(part // LANES):
        pair = slice(2 * m * LANES, 2 * (m + 1) * LANES)
        out = times(hidden0, down0_ref.at[:, pair]) + times(hidden1, down1_ref.at[:, pair])
        a, b = out[:, :LANES], out[:, LANES:]
        at = slice(m * LANES, (m + 1) * LANES)
        low = jnp.where(low_lane, a, flipped(b)).astype(BF16)
        high = jnp.where(low_lane, flipped(a), b).astype(BF16)
        out_ref[:, 0, :, at] = low.reshape(n_ep, cap, LANES)
        out_ref[:, 1, :, at] = high.reshape(n_ep, cap, LANES)


def combine_kernel(table_ref, back_ref, out_ref):
    rows = table_ref.shape[0] // 2
    half = rows // 2
    both = jnp.dot(table_ref[...], back_ref[...], preferred_element_type=F32)
    mixed = both[:rows] + both[rows:]
    low_lane = lax.broadcasted_iota(jnp.int32, (half, LANES), 1) < HALF
    for m in range(back_ref.shape[1] // LANES):
        at = slice(m * LANES, (m + 1) * LANES)
        a, b = mixed[:half, at], mixed[half:, at]
        out_ref[2 * m] = jnp.where(low_lane, a, flipped(b)).astype(BF16)
        out_ref[2 * m + 1] = jnp.where(low_lane, flipped(a), b).astype(BF16)


def total_kernel(parts_ref, out_ref):
    half = out_ref.shape[0] // 2
    total = jnp.sum(parts_ref[...].astype(F32), axis=0)
    out_ref[:half, :] = total[:, :HALF].astype(BF16)
    out_ref[half:, :] = flipped(total)[:, :HALF].astype(BF16)


def shape(dims, dtype):
    return jax.ShapeDtypeStruct(dims, dtype)


def shards(tokens, norm_gain, routes, gate_weights, expert_gate, expert_up, expert_down):
    rows, width = tokens.shape
    n_ep = lax.axis_size("ep")
    n_z = lax.axis_size("z")
    cap = rows // 2
    each = cap // 2
    slots = n_ep * cap
    mine = slots // 2
    part = width // 2
    w_gate, w_up, w_down = expert_gate[0], expert_up[0], expert_down[0]
    units = w_gate.shape[1]

    gain = norm_gain[None, :]
    picks = routes.T
    weights = gate_weights.T
    hbm = pl.BlockSpec(memory_space=pltpu.HBM)
    vmem = pl.BlockSpec(memory_space=pltpu.VMEM)
    buffer, table = pl.pallas_call(
        dispatch_kernel,
        in_specs=[hbm] * 4,
        out_shape=(shape((mine, width), BF16), shape((2 * rows, slots), BF16)),
        out_specs=(hbm, vmem),
        scratch_shapes=[
            pltpu.VMEM(tokens.shape, tokens.dtype),
            pltpu.VMEM(gain.shape, gain.dtype),
            pltpu.VMEM(picks.shape, picks.dtype),
            pltpu.VMEM(weights.shape, weights.dtype),
            pltpu.VMEM((mine, width), BF16),
            pltpu.SemaphoreType.DMA((4,)),
            pltpu.SemaphoreType.DMA((4,)),
        ],
        compiler_params=params(8),
        name="dispatch",
    )(*in_hbm(tokens, gain, picks, weights))
    received = lax.all_to_all(
        buffer.reshape(n_ep, each, width), "ep", split_axis=0, concat_axis=0, tiled=True
    ).reshape(mine, width)
    o_down = lax.ppermute(w_down, "c", SWAP)
    o_gate = lax.ppermute(w_gate, "c", SWAP)
    o_up = lax.ppermute(w_up, "c", SWAP)
    cut = width * 3 // 4
    head = pl.pallas_call(
        load_kernel,
        in_specs=[hbm],
        out_shape=shape((cut, units), BF16),
        scratch_shapes=[pltpu.SemaphoreType.DMA((1,))],
        compiler_params=params(8),
        name="load",
    )(*in_hbm(w_gate))
    hidden0, gate1, down = pl.pallas_call(
        hidden_kernel,
        in_specs=[vmem] * 2 + [hbm] * 4,
        out_shape=(
            shape((mine, units), BF16),
            shape((mine, units), F32),
            shape(w_down.shape, BF16),
        ),
        scratch_shapes=[
            pltpu.VMEM((width - cut, units), BF16),
            pltpu.VMEM(w_up.shape, BF16),
            pltpu.VMEM(w_gate.shape, BF16),
            pltpu.SemaphoreType.DMA((4,)),
        ],
        compiler_params=params(8),
        name="hidden",
    )(received, head, *in_hbm(w_gate, w_up, o_gate, w_down))
    outputs = pl.pallas_call(
        down_kernel,
        out_shape=shape((n_ep, 2, each, part), BF16),
        compiler_params=params(8),
        name="down",
    )(received, o_up, gate1, hidden0, down, o_down)
    back = lax.all_to_all(
        outputs.reshape(2 * n_ep, each, part), ("ep", "c"), split_axis=0, concat_axis=0, tiled=True
    ).reshape(slots, part)
    packed = pl.pallas_call(
        combine_kernel,
        out_shape=shape((n_z, rows // 2, LANES), BF16),
        compiler_params=params(8),
        name="combine",
    )(table, back)
    parts = lax.all_to_all(packed, "z", split_axis=0, concat_axis=0, tiled=True)
    return pl.pallas_call(
        total_kernel,
        out_shape=shape((rows, HALF), BF16),
        compiler_params=params(8),
        name="total",
    )(parts)


def solution(mesh):
    n_ep, n_tp = mesh.devices.shape
    chips = Mesh(np.asarray(mesh.devices).reshape(n_ep, n_tp // 2, 2), ("ep", "z", "c"))
    tp = ("z", "c")
    placed = (
        P("ep", None),
        P(),
        P("ep", None),
        P("ep", None),
        P("ep", None, tp),
        P("ep", None, tp),
        P("ep", tp, None),
    )
    return jax.shard_map(
        shards, mesh=chips, in_specs=placed, out_specs=P("ep", tp), check_vma=False
    )
```

```python
import jax
import jax.numpy as jnp
import numpy as np
from jax import lax
from jax.experimental import pallas as pl
from jax.experimental.pallas import tpu as pltpu
from jax.sharding import Mesh
from jax.sharding import PartitionSpec as P


WAY_IN = tuple(range(15, -1, -1))
WAY_BACK = tuple(range(31, -1, -1))
ALONG_Z = tuple((i + 10) % 16 for i in range(16))

LANES = 128
HALF = LANES // 2
F32 = jnp.float32
BF16 = jnp.bfloat16
SWAP = ((0, 1), (1, 0))


def params(mib):
    return pltpu.CompilerParams(vmem_limit_bytes=mib * 2**20)


def flipped(x):
    return pltpu.roll(x, HALF, axis=x.ndim - 1)


def column(row, eye):
    return jnp.sum(jnp.where(eye, row, 0), axis=1, keepdims=True)


def in_hbm(*arrays):
    return [pltpu.with_memory_space_constraint(x, pltpu.HBM) for x in arrays]


def started(sems, *pairs):
    copies = [pltpu.make_async_copy(src, dst, sems.at[i]) for i, (src, dst) in enumerate(pairs)]
    for copy in copies:
        copy.start()
    return copies


def slot_tables(each):
    spot = np.arange(each)
    back = np.array(WAY_BACK)
    tables = np.zeros((4, back.size * each), np.int32)
    mine = len(WAY_IN) * each
    tables[0, :mine] = np.repeat(WAY_IN, each)
    tables[1, :mine] = np.tile(spot, len(WAY_IN))
    tables[2] = np.repeat(back // 2, each)
    tables[3] = (back[:, None] % 2 * each + spot).reshape(-1)
    return tables


def dispatch_kernel(
    tok_hbm,
    picks_hbm,
    weight_hbm,
    tables_hbm,
    buffer_hbm,
    combine_ref,
    tok,
    picks,
    weight,
    tables,
    buffer,
    sems,
    out_sems,
):
    copies = started(
        sems, (tok_hbm, tok), (picks_hbm, picks), (weight_hbm, weight), (tables_hbm, tables)
    )
    rows, width = tok.shape
    mine = buffer.shape[0]
    each = rows // 4
    core = lax.axis_index("c")

    at_row = lax.broadcasted_iota(jnp.int32, (rows, rows), 0)
    at_col = lax.broadcasted_iota(jnp.int32, (rows, rows), 1)
    eye = at_row == at_col
    earlier = (at_col < at_row).astype(F32).astype(BF16)
    copies[1].wait()
    copies[2].wait()
    copies[3].wait()
    pick0 = column(picks[0:1, :], eye)
    pick1 = column(picks[1:2, :], eye)
    weight0 = column(weight[0:1, :], eye)
    weight1 = column(weight[1:2, :], eye)

    def placed(expert, place):
        is0 = pick0 == expert
        chosen = (is0 | (pick1 == expert)).astype(F32)
        rank = jnp.dot(earlier, chosen.astype(BF16), preferred_element_type=F32)
        return jnp.where(rank == place.astype(F32), chosen, 0.0), is0

    table, _ = placed(tables[0:1, :mine], tables[1:2, :mine] + core * each)
    spread = table.T.astype(BF16)
    copies[0].wait()
    chunks = out_sems.shape[0]
    leaving = []
    for i in range(chunks):
        at = pl.ds(i * (width // chunks), width // chunks)
        buffer[:, at] = jnp.dot(spread, tok[:, at], preferred_element_type=F32).astype(BF16)
        leaving.append(
            pltpu.make_async_copy(buffer.at[:, at], buffer_hbm.at[:, at], out_sems.at[i])
        )
        leaving[-1].start()
    table, is0 = placed(tables[2:3, :], tables[3:4, :])
    weights = table * jnp.where(is0, weight0, weight1)
    high = weights.astype(BF16)
    combine_ref[0:rows, :] = high
    combine_ref[rows:, :] = (weights - high.astype(F32)).astype(BF16)
    for copy in leaving:
        copy.wait()


def load_kernel(src_hbm, dst, sems):
    (copy,) = started(sems, (src_hbm.at[pl.ds(0, dst.shape[0]), :], dst))
    copy.wait()


def times(a, w):
    return jnp.dot(a, w[...], preferred_element_type=F32)


def hidden_of(gate, upper):
    return (gate / (1.0 + jnp.exp(-gate)) * upper).astype(BF16)


def hidden_kernel(
    received_ref,
    gain_ref,
    gate1,
    head0,
    gate0_hbm,
    up0_hbm,
    up1_hbm,
    down0_hbm,
    hidden_ref,
    down0_ref,
    rows_ref,
    tail0,
    up0,
    up1,
    sems,
):
    cut = head0.shape[0]
    units = up0.shape[1]
    copies = started(
        sems,
        (gate0_hbm.at[pl.ds(cut, tail0.shape[0]), :], tail0),
        (up0_hbm, up0),
        (up1_hbm, up1),
        (down0_hbm, down0_ref),
    )
    values = received_ref[...].astype(F32)
    scale = lax.rsqrt(jnp.mean(values * values, axis=-1, keepdims=True) + 1e-06)
    rows_ref[...] = (received_ref[...].astype(F32) * scale * gain_ref[...]).astype(BF16)
    gate = times(rows_ref[...], gate1)
    own = times(rows_ref[:, :cut], head0)
    copies[0].wait()
    own = own + times(rows_ref[:, cut:], tail0)
    copies[1].wait()
    hidden_ref[:, :units] = hidden_of(own, times(rows_ref[...], up0))
    copies[2].wait()
    hidden_ref[:, units:] = hidden_of(gate, times(rows_ref[...], up1))
    copies[3].wait()


def down_kernel(hidden_ref, down0_ref, down1_ref, out_ref):
    blocks, each, part = out_ref.shape
    rows, units = hidden_ref.shape[0], down0_ref.shape[0]
    low_lane = lax.broadcasted_iota(jnp.int32, (rows, LANES), 1) < HALF
    for m in range(part // LANES):
        pair = slice(2 * m * LANES, 2 * (m + 1) * LANES)
        out = times(hidden_ref[:, :units], down0_ref.at[:, pair])
        out = out + times(hidden_ref[:, units:], down1_ref.at[:, pair])
        a, b = out[:, :LANES], out[:, LANES:]
        low = jnp.where(low_lane, a, flipped(b))
        high = jnp.where(low_lane, flipped(a), b)
        for block in range(blocks):
            source, core = divmod(WAY_BACK[block], 2)
            first = WAY_IN.index(source) * each
            half = high if core else low
            out_ref[block, :, m * LANES : (m + 1) * LANES] = half[first : first + each].astype(BF16)


def combine_kernel(table_ref, back_ref, out_ref):
    rows = table_ref.shape[0] // 2
    half = rows // 2
    both = jnp.dot(table_ref[...], back_ref[...], preferred_element_type=F32)
    mixed = both[:rows] + both[rows:]
    low_lane = lax.broadcasted_iota(jnp.int32, (half, LANES), 1) < HALF
    for m in range(back_ref.shape[1] // LANES):
        at = slice(m * LANES, (m + 1) * LANES)
        a, b = mixed[:half, at], mixed[half:, at]
        out_ref[ALONG_Z.index(2 * m)] = jnp.where(low_lane, a, flipped(b)).astype(BF16)
        out_ref[ALONG_Z.index(2 * m + 1)] = jnp.where(low_lane, flipped(a), b).astype(BF16)


def total_kernel(parts_ref, out_ref):
    half = out_ref.shape[0] // 2
    total = jnp.sum(parts_ref[...].astype(F32), axis=0)
    out_ref[:half, :] = total[:, :HALF].astype(BF16)
    out_ref[half:, :] = flipped(total)[:, :HALF].astype(BF16)


def shape(dims, dtype):
    return jax.ShapeDtypeStruct(dims, dtype)


def shards(tokens, norm_gain, routes, gate_weights, expert_gate, expert_up, expert_down):
    rows, width = tokens.shape
    n_ep = lax.axis_size("ep")
    n_z = lax.axis_size("z")
    cap = rows // 2
    each = cap // 2
    slots = n_ep * cap
    mine = slots // 2
    part = width // 2
    w_gate, w_up, w_down = expert_gate[0], expert_up[0], expert_down[0]
    units = w_gate.shape[1]

    gain = norm_gain[None, :]
    picks = routes.T
    weights = gate_weights.T
    tables = jnp.asarray(slot_tables(each))
    hbm = pl.BlockSpec(memory_space=pltpu.HBM)
    vmem = pl.BlockSpec(memory_space=pltpu.VMEM)
    buffer, table = pl.pallas_call(
        dispatch_kernel,
        in_specs=[hbm] * 4,
        out_shape=(shape((mine, width), BF16), shape((2 * rows, slots), BF16)),
        out_specs=(hbm, vmem),
        scratch_shapes=[
            pltpu.VMEM(tokens.shape, tokens.dtype),
            pltpu.VMEM(picks.shape, picks.dtype),
            pltpu.VMEM(weights.shape, weights.dtype),
            pltpu.VMEM(tables.shape, tables.dtype),
            pltpu.VMEM((mine, width), BF16),
            pltpu.SemaphoreType.DMA((4,)),
            pltpu.SemaphoreType.DMA((4,)),
        ],
        compiler_params=params(8),
        name="dispatch",
    )(*in_hbm(tokens, picks, weights, tables))
    received = lax.all_to_all(
        buffer.reshape(n_ep, each, width), "ep", split_axis=0, concat_axis=0, tiled=True, axis_index_groups=[WAY_IN]
    ).reshape(mine, width)
    o_down = lax.ppermute(w_down, "c", SWAP)
    o_gate = lax.ppermute(w_gate, "c", SWAP)
    o_up = lax.ppermute(w_up, "c", SWAP)
    cut = width * 3 // 4
    head = pl.pallas_call(
        load_kernel,
        in_specs=[hbm],
        out_shape=shape((cut, units), BF16),
        scratch_shapes=[pltpu.SemaphoreType.DMA((1,))],
        compiler_params=params(8),
        name="load",
    )(*in_hbm(w_gate))
    hidden, down = pl.pallas_call(
        hidden_kernel,
        in_specs=[vmem] * 4 + [hbm] * 4,
        out_shape=(shape((mine, 2 * units), BF16), shape(w_down.shape, BF16)),
        scratch_shapes=[
            pltpu.VMEM((mine, width), BF16),
            pltpu.VMEM((width - cut, units), BF16),
            pltpu.VMEM(w_up.shape, BF16),
            pltpu.VMEM(w_up.shape, BF16),
            pltpu.SemaphoreType.DMA((4,)),
        ],
        compiler_params=params(8),
        name="hidden",
    )(received, gain, o_gate, head, *in_hbm(w_gate, w_up, o_up, w_down))
    outputs = pl.pallas_call(
        down_kernel,
        out_shape=shape((2 * n_ep, each, part), BF16),
        compiler_params=params(8),
        name="down",
    )(hidden, down, o_down)
    back = lax.all_to_all(
        outputs, ("ep", "c"), split_axis=0, concat_axis=0, tiled=True, axis_index_groups=[WAY_BACK]
    ).reshape(slots, part)
    packed = pl.pallas_call(
        combine_kernel,
        out_shape=shape((n_z, rows // 2, LANES), BF16),
        compiler_params=params(8),
        name="combine",
    )(table, back)
    parts = lax.all_to_all(packed, "z", split_axis=0, concat_axis=0, tiled=True, axis_index_groups=[ALONG_Z])
    return pl.pallas_call(
        total_kernel,
        out_shape=shape((rows, HALF), BF16),
        compiler_params=params(8),
        name="total",
    )(parts)


def solution(mesh):
    n_ep, n_tp = mesh.devices.shape
    chips = Mesh(np.asarray(mesh.devices).reshape(n_ep, n_tp // 2, 2), ("ep", "z", "c"))
    tp = ("z", "c")
    placed = (
        P("ep", None),
        P(),
        P("ep", None),
        P("ep", None),
        P("ep", None, tp),
        P("ep", None, tp),
        P("ep", tp, None),
    )
    return jax.shard_map(
        shards, mesh=chips, in_specs=placed, out_specs=P("ep", tp), check_vma=False
    )
```

```python
import jax
import jax.numpy as jnp
import numpy as np
from jax import lax
from jax.experimental import pallas as pl
from jax.experimental.pallas import tpu as pltpu
from jax.sharding import Mesh
from jax.sharding import PartitionSpec as P


SIDE = 4


def hops(chip):
    y, x = divmod(chip, SIDE)
    return min(y, SIDE - y) + min(x, SIDE - x)


WAY_IN = tuple(range(15, -1, -1))
WAY_BACK = tuple(
    2 * chip + core for chip in sorted(range(16), key=lambda e: (-hops(e), e)) for core in (1, 0)
)
ALONG_Z = tuple((i + 10) % 16 for i in range(16))


LANES = 128
HALF = LANES // 2
F32 = jnp.float32
BF16 = jnp.bfloat16
SWAP = ((0, 1), (1, 0))


def params(mib):
    return pltpu.CompilerParams(vmem_limit_bytes=mib * 2**20)


def flipped(x):
    return pltpu.roll(x, HALF, axis=x.ndim - 1)


def column(row, eye):
    return jnp.sum(jnp.where(eye, row, 0), axis=1, keepdims=True)


def in_hbm(*arrays):
    return [pltpu.with_memory_space_constraint(x, pltpu.HBM) for x in arrays]


def started(sems, *pairs):
    copies = [pltpu.make_async_copy(src, dst, sems.at[i]) for i, (src, dst) in enumerate(pairs)]
    for copy in copies:
        copy.start()
    return copies


def slot_tables(each):
    chip, core = np.divmod(np.array(WAY_BACK), 2)
    rank = core[:, None] * each + np.arange(each)
    return np.stack([np.repeat(chip, each), rank.reshape(-1)]).astype(np.int32)


def dispatch_kernel(
    tok_hbm,
    picks_hbm,
    weight_hbm,
    tables_hbm,
    buffer_hbm,
    combine_ref,
    tok,
    picks,
    weight,
    tables,
    buffer,
    sems,
    out_sems,
):
    copies = started(
        sems, (tok_hbm, tok), (picks_hbm, picks), (weight_hbm, weight), (tables_hbm, tables)
    )
    rows, width = tok.shape
    mine = buffer.shape[0]
    each = rows // 4
    half = lax.axis_index("c")

    at_row = lax.broadcasted_iota(jnp.int32, (rows, rows), 0)
    at_col = lax.broadcasted_iota(jnp.int32, (rows, rows), 1)
    eye = at_row == at_col
    before = (at_row < at_col).astype(F32).astype(BF16)
    slot = lax.broadcasted_iota(jnp.int32, (mine, rows), 0)
    expert = len(WAY_IN) - 1 - slot // each
    place = (slot % each + half * each).astype(F32)
    copies[1].wait()
    chosen = ((picks[0:1, :] == expert) | (picks[1:2, :] == expert)).astype(F32)
    rank = jnp.dot(chosen.astype(BF16), before, preferred_element_type=F32)
    spread = jnp.where(rank == place, chosen, 0.0).astype(BF16)
    copies[0].wait()
    chunks = out_sems.shape[0]
    leaving = []
    for i in range(chunks):
        at = pl.ds(i * (width // chunks), width // chunks)
        buffer[:, at] = jnp.dot(spread, tok[:, at], preferred_element_type=F32).astype(BF16)
        leaving.append(
            pltpu.make_async_copy(buffer.at[:, at], buffer_hbm.at[:, at], out_sems.at[i])
        )
        leaving[-1].start()
    copies[2].wait()
    copies[3].wait()
    pick0 = column(picks[0:1, :], eye)
    pick1 = column(picks[1:2, :], eye)
    weight0 = column(weight[0:1, :], eye)
    weight1 = column(weight[1:2, :], eye)
    earlier = (at_col < at_row).astype(F32).astype(BF16)
    is0 = pick0 == tables[0:1, :]
    chosen = (is0 | (pick1 == tables[0:1, :])).astype(F32)
    rank = jnp.dot(earlier, chosen.astype(BF16), preferred_element_type=F32)
    table = jnp.where(rank == tables[1:2, :].astype(F32), chosen, 0.0)
    weights = table * jnp.where(is0, weight0, weight1)
    high = weights.astype(BF16)
    combine_ref[0:rows, :] = high
    combine_ref[rows:, :] = (weights - high.astype(F32)).astype(BF16)
    for copy in leaving:
        copy.wait()


def load_kernel(src_hbm, dst, sems):
    (copy,) = started(sems, (src_hbm.at[pl.ds(0, dst.shape[0]), :], dst))
    copy.wait()


def times(a, w):
    return jnp.dot(a, w[...], preferred_element_type=F32)


def hidden_of(gate, upper):
    return (gate / (1.0 + jnp.exp(-gate)) * upper).astype(BF16)


def hidden_kernel(
    received_ref,
    gain_ref,
    gate1,
    head0,
    gate0_hbm,
    up0_hbm,
    up1_hbm,
    down0_hbm,
    hidden_ref,
    down0_ref,
    rows_ref,
    tail0,
    up0,
    up1,
    sems,
):
    cut = head0.shape[0]
    units = up0.shape[1]
    copies = started(
        sems,
        (gate0_hbm.at[pl.ds(cut, tail0.shape[0]), :], tail0),
        (up0_hbm, up0),
        (up1_hbm, up1),
        (down0_hbm, down0_ref),
    )
    values = received_ref[...].astype(F32)
    scale = lax.rsqrt(jnp.mean(values * values, axis=-1, keepdims=True) + 1e-06)
    rows_ref[...] = (received_ref[...].astype(F32) * scale * gain_ref[...]).astype(BF16)
    gate = times(rows_ref[...], gate1)
    own = times(rows_ref[:, :cut], head0)
    copies[0].wait()
    own = own + times(rows_ref[:, cut:], tail0)
    copies[1].wait()
    hidden_ref[:, :units] = hidden_of(own, times(rows_ref[...], up0))
    copies[2].wait()
    hidden_ref[:, units:] = hidden_of(gate, times(rows_ref[...], up1))
    copies[3].wait()


def down_kernel(hidden_ref, down0_ref, down1_ref, out_ref):
    blocks, each, part = out_ref.shape
    rows, units = hidden_ref.shape[0], down0_ref.shape[0]
    low_lane = lax.broadcasted_iota(jnp.int32, (rows, LANES), 1) < HALF
    for m in range(part // LANES):
        pair = slice(2 * m * LANES, 2 * (m + 1) * LANES)
        out = times(hidden_ref[:, :units], down0_ref.at[:, pair])
        out = out + times(hidden_ref[:, units:], down1_ref.at[:, pair])
        a, b = out[:, :LANES], out[:, LANES:]
        low = jnp.where(low_lane, a, flipped(b))
        high = jnp.where(low_lane, flipped(a), b)
        for block in range(blocks):
            source, core = divmod(WAY_BACK[block], 2)
            first = WAY_IN.index(source) * each
            half = high if core else low
            out_ref[block, :, m * LANES : (m + 1) * LANES] = half[first : first + each].astype(BF16)


def combine_kernel(table_ref, back_ref, out_ref):
    rows = table_ref.shape[0] // 2
    half = rows // 2
    both = jnp.dot(table_ref[...], back_ref[...], preferred_element_type=F32)
    mixed = both[:rows] + both[rows:]
    low_lane = lax.broadcasted_iota(jnp.int32, (half, LANES), 1) < HALF
    for m in range(back_ref.shape[1] // LANES):
        at = slice(m * LANES, (m + 1) * LANES)
        a, b = mixed[:half, at], mixed[half:, at]
        out_ref[ALONG_Z.index(2 * m)] = jnp.where(low_lane, a, flipped(b)).astype(BF16)
        out_ref[ALONG_Z.index(2 * m + 1)] = jnp.where(low_lane, flipped(a), b).astype(BF16)


def total_kernel(parts_ref, out_ref):
    half = out_ref.shape[0] // 2
    total = jnp.sum(parts_ref[...].astype(F32), axis=0)
    out_ref[:half, :] = total[:, :HALF].astype(BF16)
    out_ref[half:, :] = flipped(total)[:, :HALF].astype(BF16)


def shape(dims, dtype):
    return jax.ShapeDtypeStruct(dims, dtype)


def shards(tokens, norm_gain, routes, gate_weights, expert_gate, expert_up, expert_down):
    rows, width = tokens.shape
    n_ep = lax.axis_size("ep")
    n_z = lax.axis_size("z")
    cap = rows // 2
    each = cap // 2
    slots = n_ep * cap
    mine = slots // 2
    part = width // 2
    w_gate, w_up, w_down = expert_gate[0], expert_up[0], expert_down[0]
    units = w_gate.shape[1]

    gain = norm_gain[None, :]
    picks = routes.T
    weights = gate_weights.T
    tables = jnp.asarray(slot_tables(each))
    hbm = pl.BlockSpec(memory_space=pltpu.HBM)
    vmem = pl.BlockSpec(memory_space=pltpu.VMEM)
    buffer, table = pl.pallas_call(
        dispatch_kernel,
        in_specs=[hbm] * 4,
        out_shape=(shape((mine, width), BF16), shape((2 * rows, slots), BF16)),
        out_specs=(hbm, vmem),
        scratch_shapes=[
            pltpu.VMEM(tokens.shape, tokens.dtype),
            pltpu.VMEM(picks.shape, picks.dtype),
            pltpu.VMEM(weights.shape, weights.dtype),
            pltpu.VMEM(tables.shape, tables.dtype),
            pltpu.VMEM((mine, width), BF16),
            pltpu.SemaphoreType.DMA((4,)),
            pltpu.SemaphoreType.DMA((4,)),
        ],
        compiler_params=params(8),
        name="dispatch",
    )(*in_hbm(tokens, picks, weights, tables))
    received = lax.all_to_all(
        buffer.reshape(n_ep, each, width),
        "ep",
        split_axis=0,
        concat_axis=0,
        tiled=True,
        axis_index_groups=[WAY_IN],
    ).reshape(mine, width)
    o_down = lax.ppermute(w_down, "c", SWAP)
    o_gate = lax.ppermute(w_gate, "c", SWAP)
    o_up = lax.ppermute(w_up, "c", SWAP)
    cut = width * 3 // 4
    head = pl.pallas_call(
        load_kernel,
        in_specs=[hbm],
        out_shape=shape((cut, units), BF16),
        scratch_shapes=[pltpu.SemaphoreType.DMA((1,))],
        compiler_params=params(8),
        name="load",
    )(*in_hbm(w_gate))
    hidden, down = pl.pallas_call(
        hidden_kernel,
        in_specs=[vmem] * 4 + [hbm] * 4,
        out_shape=(shape((mine, 2 * units), BF16), shape(w_down.shape, BF16)),
        scratch_shapes=[
            pltpu.VMEM((mine, width), BF16),
            pltpu.VMEM((width - cut, units), BF16),
            pltpu.VMEM(w_up.shape, BF16),
            pltpu.VMEM(w_up.shape, BF16),
            pltpu.SemaphoreType.DMA((4,)),
        ],
        compiler_params=params(8),
        name="hidden",
    )(received, gain, o_gate, head, *in_hbm(w_gate, w_up, o_up, w_down))
    outputs = pl.pallas_call(
        down_kernel,
        out_shape=shape((2 * n_ep, each, part), BF16),
        compiler_params=params(8),
        name="down",
    )(hidden, down, o_down)
    back = lax.all_to_all(
        outputs, ("ep", "c"), split_axis=0, concat_axis=0, tiled=True, axis_index_groups=[WAY_BACK]
    ).reshape(slots, part)
    packed = pl.pallas_call(
        combine_kernel,
        out_shape=shape((n_z, rows // 2, LANES), BF16),
        compiler_params=params(8),
        name="combine",
    )(table, back)
    parts = lax.all_to_all(packed, "z", split_axis=0, concat_axis=0, tiled=True, axis_index_groups=[ALONG_Z])
    return pl.pallas_call(
        total_kernel,
        out_shape=shape((rows, HALF), BF16),
        compiler_params=params(8),
        name="total",
    )(parts)


def solution(mesh):
    n_ep, n_tp = mesh.devices.shape
    chips = Mesh(np.asarray(mesh.devices).reshape(n_ep, n_tp // 2, 2), ("ep", "z", "c"))
    tp = ("z", "c")
    placed = (
        P("ep", None),
        P(),
        P("ep", None),
        P("ep", None),
        P("ep", None, tp),
        P("ep", None, tp),
        P("ep", tp, None),
    )
    return jax.shard_map(
        shards, mesh=chips, in_specs=placed, out_specs=P("ep", tp), check_vma=False
    )
```

```python
import jax
import jax.numpy as jnp
import numpy as np
from jax import lax
from jax.experimental import pallas as pl
from jax.experimental.pallas import tpu as pltpu
from jax.sharding import Mesh
from jax.sharding import PartitionSpec as P


SIDE = 4


def hops(chip):
    y, x = divmod(chip, SIDE)
    return min(y, SIDE - y) + min(x, SIDE - x)


WAY_IN = tuple(sorted(range(16), key=lambda e: (-hops(e), -e)))
WAY_BACK = tuple(
    2 * chip + core for chip in sorted(range(16), key=lambda e: (-hops(e), e)) for core in (1, 0)
)
ALONG_Z = tuple((i + 10) % 16 for i in range(16))


LANES = 128
HALF = LANES // 2
F32 = jnp.float32
BF16 = jnp.bfloat16
SWAP = ((0, 1), (1, 0))


def params(mib):
    return pltpu.CompilerParams(vmem_limit_bytes=mib * 2**20)


def flipped(x):
    return pltpu.roll(x, HALF, axis=x.ndim - 1)


def column(row, eye):
    return jnp.sum(jnp.where(eye, row, 0), axis=1, keepdims=True)


def in_hbm(*arrays):
    return [pltpu.with_memory_space_constraint(x, pltpu.HBM) for x in arrays]


def started(sems, *pairs):
    copies = [pltpu.make_async_copy(src, dst, sems.at[i]) for i, (src, dst) in enumerate(pairs)]
    for copy in copies:
        copy.start()
    return copies


def slot_tables(each):
    chip, core = np.divmod(np.array(WAY_BACK), 2)
    rank = core[:, None] * each + np.arange(each)
    return np.stack([np.repeat(chip, each), rank.reshape(-1)]).astype(np.int32)


def dispatch_kernel(
    tok_hbm,
    picks_hbm,
    weight_hbm,
    tables_hbm,
    buffer_hbm,
    combine_ref,
    tok,
    picks,
    weight,
    tables,
    buffer,
    sems,
    out_sems,
):
    copies = started(
        sems, (tok_hbm, tok), (picks_hbm, picks), (weight_hbm, weight), (tables_hbm, tables)
    )
    rows, width = tok.shape
    mine = buffer.shape[0]
    each = rows // 4
    half = lax.axis_index("c")

    at_row = lax.broadcasted_iota(jnp.int32, (rows, rows), 0)
    at_col = lax.broadcasted_iota(jnp.int32, (rows, rows), 1)
    eye = at_row == at_col
    before = (at_row < at_col).astype(F32).astype(BF16)
    slot = lax.broadcasted_iota(jnp.int32, (mine, rows), 0)
    expert = jnp.zeros_like(slot)
    for block, chip in enumerate(WAY_IN):
        expert = jnp.where(slot // each == block, chip, expert)
    place = (slot % each + half * each).astype(F32)
    copies[1].wait()
    chosen = ((picks[0:1, :] == expert) | (picks[1:2, :] == expert)).astype(F32)
    rank = jnp.dot(chosen.astype(BF16), before, preferred_element_type=F32)
    spread = jnp.where(rank == place, chosen, 0.0).astype(BF16)
    copies[0].wait()
    chunks = out_sems.shape[0]
    leaving = []
    for i in range(chunks):
        at = pl.ds(i * (width // chunks), width // chunks)
        buffer[:, at] = jnp.dot(spread, tok[:, at], preferred_element_type=F32).astype(BF16)
        leaving.append(
            pltpu.make_async_copy(buffer.at[:, at], buffer_hbm.at[:, at], out_sems.at[i])
        )
        leaving[-1].start()
    copies[2].wait()
    copies[3].wait()
    pick0 = column(picks[0:1, :], eye)
    pick1 = column(picks[1:2, :], eye)
    weight0 = column(weight[0:1, :], eye)
    weight1 = column(weight[1:2, :], eye)
    earlier = (at_col < at_row).astype(F32).astype(BF16)
    is0 = pick0 == tables[0:1, :]
    chosen = (is0 | (pick1 == tables[0:1, :])).astype(F32)
    rank = jnp.dot(earlier, chosen.astype(BF16), preferred_element_type=F32)
    table = jnp.where(rank == tables[1:2, :].astype(F32), chosen, 0.0)
    weights = table * jnp.where(is0, weight0, weight1)
    high = weights.astype(BF16)
    combine_ref[0:rows, :] = high
    combine_ref[rows:, :] = (weights - high.astype(F32)).astype(BF16)
    for copy in leaving:
        copy.wait()


def load_kernel(src_hbm, dst, sems):
    (copy,) = started(sems, (src_hbm.at[pl.ds(0, dst.shape[0]), :], dst))
    copy.wait()


def times(a, w):
    return jnp.dot(a, w[...], preferred_element_type=F32)


def hidden_of(gate, upper):
    return (gate / (1.0 + jnp.exp(-gate)) * upper).astype(BF16)


def hidden_kernel(
    received_ref,
    gain_ref,
    gate1,
    head0,
    gate0_hbm,
    up0_hbm,
    up1_hbm,
    down0_hbm,
    hidden_ref,
    down0_ref,
    rows_ref,
    tail0,
    up0,
    up1,
    sems,
):
    cut = head0.shape[0]
    units = up0.shape[1]
    copies = started(
        sems,
        (gate0_hbm.at[pl.ds(cut, tail0.shape[0]), :], tail0),
        (up0_hbm, up0),
        (up1_hbm, up1),
        (down0_hbm, down0_ref),
    )
    values = received_ref[...].astype(F32)
    scale = lax.rsqrt(jnp.mean(values * values, axis=-1, keepdims=True) + 1e-06)
    rows_ref[...] = (received_ref[...].astype(F32) * scale * gain_ref[...]).astype(BF16)
    gate = times(rows_ref[...], gate1)
    own = times(rows_ref[:, :cut], head0)
    copies[0].wait()
    own = own + times(rows_ref[:, cut:], tail0)
    copies[1].wait()
    hidden_ref[:, :units] = hidden_of(own, times(rows_ref[...], up0))
    copies[2].wait()
    hidden_ref[:, units:] = hidden_of(gate, times(rows_ref[...], up1))
    copies[3].wait()


def down_kernel(hidden_ref, down0_ref, down1_ref, out_ref):
    blocks, each, part = out_ref.shape
    rows, units = hidden_ref.shape[0], down0_ref.shape[0]
    low_lane = lax.broadcasted_iota(jnp.int32, (rows, LANES), 1) < HALF
    for m in range(part // LANES):
        pair = slice(2 * m * LANES, 2 * (m + 1) * LANES)
        out = times(hidden_ref[:, :units], down0_ref.at[:, pair])
        out = out + times(hidden_ref[:, units:], down1_ref.at[:, pair])
        a, b = out[:, :LANES], out[:, LANES:]
        low = jnp.where(low_lane, a, flipped(b))
        high = jnp.where(low_lane, flipped(a), b)
        for block in range(blocks):
            source, core = divmod(WAY_BACK[block], 2)
            first = WAY_IN.index(source) * each
            half = high if core else low
            out_ref[block, :, m * LANES : (m + 1) * LANES] = half[first : first + each].astype(BF16)


def combine_kernel(table_ref, back_ref, out_ref):
    rows = table_ref.shape[0] // 2
    half = rows // 2
    both = jnp.dot(table_ref[...], back_ref[...], preferred_element_type=F32)
    mixed = both[:rows] + both[rows:]
    low_lane = lax.broadcasted_iota(jnp.int32, (half, LANES), 1) < HALF
    for m in range(back_ref.shape[1] // LANES):
        at = slice(m * LANES, (m + 1) * LANES)
        a, b = mixed[:half, at], mixed[half:, at]
        out_ref[ALONG_Z.index(2 * m)] = jnp.where(low_lane, a, flipped(b)).astype(BF16)
        out_ref[ALONG_Z.index(2 * m + 1)] = jnp.where(low_lane, flipped(a), b).astype(BF16)


def total_kernel(parts_ref, out_ref):
    half = out_ref.shape[0] // 2
    total = jnp.sum(parts_ref[...].astype(F32), axis=0)
    out_ref[:half, :] = total[:, :HALF].astype(BF16)
    out_ref[half:, :] = flipped(total)[:, :HALF].astype(BF16)


def shape(dims, dtype):
    return jax.ShapeDtypeStruct(dims, dtype)


def shards(tokens, norm_gain, routes, gate_weights, expert_gate, expert_up, expert_down):
    rows, width = tokens.shape
    n_ep = lax.axis_size("ep")
    n_z = lax.axis_size("z")
    cap = rows // 2
    each = cap // 2
    slots = n_ep * cap
    mine = slots // 2
    part = width // 2
    w_gate, w_up, w_down = expert_gate[0], expert_up[0], expert_down[0]
    units = w_gate.shape[1]

    gain = norm_gain[None, :]
    picks = routes.T
    weights = gate_weights.T
    tables = jnp.asarray(slot_tables(each))
    hbm = pl.BlockSpec(memory_space=pltpu.HBM)
    vmem = pl.BlockSpec(memory_space=pltpu.VMEM)
    buffer, table = pl.pallas_call(
        dispatch_kernel,
        in_specs=[hbm] * 4,
        out_shape=(shape((mine, width), BF16), shape((2 * rows, slots), BF16)),
        out_specs=(hbm, vmem),
        scratch_shapes=[
            pltpu.VMEM(tokens.shape, tokens.dtype),
            pltpu.VMEM(picks.shape, picks.dtype),
            pltpu.VMEM(weights.shape, weights.dtype),
            pltpu.VMEM(tables.shape, tables.dtype),
            pltpu.VMEM((mine, width), BF16),
            pltpu.SemaphoreType.DMA((4,)),
            pltpu.SemaphoreType.DMA((4,)),
        ],
        compiler_params=params(8),
        name="dispatch",
    )(*in_hbm(tokens, picks, weights, tables))
    received = lax.all_to_all(
        buffer.reshape(n_ep, each, width),
        "ep",
        split_axis=0,
        concat_axis=0,
        tiled=True,
        axis_index_groups=[WAY_IN],
    ).reshape(mine, width)
    o_down = lax.ppermute(w_down, "c", SWAP)
    o_gate = lax.ppermute(w_gate, "c", SWAP)
    o_up = lax.ppermute(w_up, "c", SWAP)
    cut = width * 3 // 4
    head = pl.pallas_call(
        load_kernel,
        in_specs=[hbm],
        out_shape=shape((cut, units), BF16),
        scratch_shapes=[pltpu.SemaphoreType.DMA((1,))],
        compiler_params=params(8),
        name="load",
    )(*in_hbm(w_gate))
    hidden, down = pl.pallas_call(
        hidden_kernel,
        in_specs=[vmem] * 4 + [hbm] * 4,
        out_shape=(shape((mine, 2 * units), BF16), shape(w_down.shape, BF16)),
        scratch_shapes=[
            pltpu.VMEM((mine, width), BF16),
            pltpu.VMEM((width - cut, units), BF16),
            pltpu.VMEM(w_up.shape, BF16),
            pltpu.VMEM(w_up.shape, BF16),
            pltpu.SemaphoreType.DMA((4,)),
        ],
        compiler_params=params(8),
        name="hidden",
    )(received, gain, o_gate, head, *in_hbm(w_gate, w_up, o_up, w_down))
    outputs = pl.pallas_call(
        down_kernel,
        out_shape=shape((2 * n_ep, each, part), BF16),
        compiler_params=params(8),
        name="down",
    )(hidden, down, o_down)
    back = lax.all_to_all(
        outputs, ("ep", "c"), split_axis=0, concat_axis=0, tiled=True, axis_index_groups=[WAY_BACK]
    ).reshape(slots, part)
    packed = pl.pallas_call(
        combine_kernel,
        out_shape=shape((n_z, rows // 2, LANES), BF16),
        compiler_params=params(8),
        name="combine",
    )(table, back)
    parts = lax.all_to_all(packed, "z", split_axis=0, concat_axis=0, tiled=True, axis_index_groups=[ALONG_Z])
    return pl.pallas_call(
        total_kernel,
        out_shape=shape((rows, HALF), BF16),
        compiler_params=params(8),
        name="total",
    )(parts)


def solution(mesh):
    n_ep, n_tp = mesh.devices.shape
    chips = Mesh(np.asarray(mesh.devices).reshape(n_ep, n_tp // 2, 2), ("ep", "z", "c"))
    tp = ("z", "c")
    placed = (
        P("ep", None),
        P(),
        P("ep", None),
        P("ep", None),
        P("ep", None, tp),
        P("ep", None, tp),
        P("ep", tp, None),
    )
    return jax.shard_map(
        shards, mesh=chips, in_specs=placed, out_specs=P("ep", tp), check_vma=False
    )
```

```python
import jax
import jax.numpy as jnp
import numpy as np
from jax import lax
from jax.experimental import pallas as pl
from jax.experimental.pallas import tpu as pltpu
from jax.sharding import Mesh
from jax.sharding import PartitionSpec as P


SIDE = 4


def hops(chip):
    y, x = divmod(chip, SIDE)
    return min(y, SIDE - y) + min(x, SIDE - x)


WAY_IN = tuple(sorted(range(16), key=lambda e: (-hops(e), -e)))
WAY_BACK = tuple(
    2 * chip + core for chip in sorted(range(16), key=lambda e: (-hops(e), e)) for core in (1, 0)
)
ALONG_Z = tuple((i + 10) % 16 for i in range(16))


LANES = 128
HALF = LANES // 2
F32 = jnp.float32
BF16 = jnp.bfloat16
SWAP = ((0, 1), (1, 0))


def params(mib):
    return pltpu.CompilerParams(vmem_limit_bytes=mib * 2**20)


def flipped(x):
    return pltpu.roll(x, HALF, axis=x.ndim - 1)


def column(row, eye):
    return jnp.sum(jnp.where(eye, row, 0), axis=1, keepdims=True)


def in_hbm(*arrays):
    return [pltpu.with_memory_space_constraint(x, pltpu.HBM) for x in arrays]


def started(sems, *pairs):
    copies = [pltpu.make_async_copy(src, dst, sems.at[i]) for i, (src, dst) in enumerate(pairs)]
    for copy in copies:
        copy.start()
    return copies


def slot_tables(each):
    chip, core = np.divmod(np.array(WAY_BACK), 2)
    rank = core[:, None] * each + np.arange(each)
    return np.stack([np.repeat(chip, each), rank.reshape(-1)]).astype(np.int32)


def dispatch_kernel(
    tok_hbm,
    picks_hbm,
    weight_hbm,
    tables_hbm,
    buffer_hbm,
    combine_ref,
    tok,
    picks,
    weight,
    tables,
    buffer,
    sems,
    out_sems,
):
    copies = started(
        sems, (tok_hbm, tok), (picks_hbm, picks), (weight_hbm, weight), (tables_hbm, tables)
    )
    rows, width = tok.shape
    mine = buffer.shape[0]
    each = rows // 4
    half = lax.axis_index("c")

    at_row = lax.broadcasted_iota(jnp.int32, (rows, rows), 0)
    at_col = lax.broadcasted_iota(jnp.int32, (rows, rows), 1)
    eye = at_row == at_col
    before = (at_row < at_col).astype(F32).astype(BF16)
    slot = lax.broadcasted_iota(jnp.int32, (mine, rows), 0)
    expert = jnp.zeros_like(slot)
    for block, chip in enumerate(WAY_IN):
        expert = jnp.where(slot // each == block, chip, expert)
    place = (slot % each + half * each).astype(F32)
    copies[1].wait()
    chosen = ((picks[0:1, :] == expert) | (picks[1:2, :] == expert)).astype(F32)
    rank = jnp.dot(chosen.astype(BF16), before, preferred_element_type=F32)
    spread = jnp.where(rank == place, chosen, 0.0).astype(BF16)
    copies[0].wait()
    chunks = out_sems.shape[0]
    leaving = []
    for i in range(chunks):
        at = pl.ds(i * (width // chunks), width // chunks)
        buffer[:, at] = jnp.dot(spread, tok[:, at], preferred_element_type=F32).astype(BF16)
        leaving.append(
            pltpu.make_async_copy(buffer.at[:, at], buffer_hbm.at[:, at], out_sems.at[i])
        )
        leaving[-1].start()
    copies[2].wait()
    copies[3].wait()
    pick0 = column(picks[0:1, :], eye)
    pick1 = column(picks[1:2, :], eye)
    weight0 = column(weight[0:1, :], eye)
    weight1 = column(weight[1:2, :], eye)
    earlier = (at_col < at_row).astype(F32).astype(BF16)
    is0 = pick0 == tables[0:1, :]
    chosen = (is0 | (pick1 == tables[0:1, :])).astype(F32)
    rank = jnp.dot(earlier, chosen.astype(BF16), preferred_element_type=F32)
    table = jnp.where(rank == tables[1:2, :].astype(F32), chosen, 0.0)
    weights = table * jnp.where(is0, weight0, weight1)
    high = weights.astype(BF16)
    combine_ref[0:rows, :] = high
    combine_ref[rows:, :] = (weights - high.astype(F32)).astype(BF16)
    for copy in leaving:
        copy.wait()


def load_kernel(src_hbm, dst, sems):
    (copy,) = started(sems, (src_hbm.at[pl.ds(0, dst.shape[0]), :], dst))
    copy.wait()


def times(a, w):
    return jnp.dot(a, w[...], preferred_element_type=F32)


def hidden_of(gate, upper):
    return (gate / (1.0 + jnp.exp(-gate)) * upper).astype(BF16)


def hidden_kernel(
    received_ref,
    gain_ref,
    head0,
    gate0_hbm,
    up0_hbm,
    gate1_hbm,
    up1_hbm,
    hidden_ref,
    rows_ref,
    tail0,
    up0,
    gate1,
    up1,
    sems,
):
    cut = head0.shape[0]
    units = up0.shape[1]
    copies = started(
        sems,
        (gate0_hbm.at[pl.ds(cut, tail0.shape[0]), :], tail0),
        (up0_hbm, up0),
        (gate1_hbm, gate1),
        (up1_hbm, up1),
    )
    values = received_ref[...].astype(F32)
    scale = lax.rsqrt(jnp.mean(values * values, axis=-1, keepdims=True) + 1e-06)
    rows_ref[...] = (received_ref[...].astype(F32) * scale * gain_ref[...]).astype(BF16)
    own = times(rows_ref[:, :cut], head0)
    copies[0].wait()
    own = own + times(rows_ref[:, cut:], tail0)
    copies[1].wait()
    hidden_ref[:, :units] = hidden_of(own, times(rows_ref[...], up0))
    copies[2].wait()
    gate = times(rows_ref[...], gate1)
    copies[3].wait()
    hidden_ref[:, units:] = hidden_of(gate, times(rows_ref[...], up1))


def down_kernel(hidden_ref, down0_ref, down1_ref, out_ref):
    blocks, each, part = out_ref.shape
    rows, units = hidden_ref.shape[0], down0_ref.shape[0]
    low_lane = lax.broadcasted_iota(jnp.int32, (rows, LANES), 1) < HALF
    for m in range(part // LANES):
        pair = slice(2 * m * LANES, 2 * (m + 1) * LANES)
        out = times(hidden_ref[:, :units], down0_ref.at[:, pair])
        out = out + times(hidden_ref[:, units:], down1_ref.at[:, pair])
        a, b = out[:, :LANES], out[:, LANES:]
        low = jnp.where(low_lane, a, flipped(b))
        high = jnp.where(low_lane, flipped(a), b)
        for block in range(blocks):
            source, core = divmod(WAY_BACK[block], 2)
            first = WAY_IN.index(source) * each
            half = high if core else low
            out_ref[block, :, m * LANES : (m + 1) * LANES] = half[first : first + each].astype(BF16)


def combine_kernel(table_ref, back_ref, out_ref):
    rows = table_ref.shape[0] // 2
    half = rows // 2
    both = jnp.dot(table_ref[...], back_ref[...], preferred_element_type=F32)
    mixed = both[:rows] + both[rows:]
    low_lane = lax.broadcasted_iota(jnp.int32, (half, LANES), 1) < HALF
    for m in range(back_ref.shape[1] // LANES):
        at = slice(m * LANES, (m + 1) * LANES)
        a, b = mixed[:half, at], mixed[half:, at]
        out_ref[ALONG_Z.index(2 * m)] = jnp.where(low_lane, a, flipped(b)).astype(BF16)
        out_ref[ALONG_Z.index(2 * m + 1)] = jnp.where(low_lane, flipped(a), b).astype(BF16)


def total_kernel(parts_ref, out_ref):
    half = out_ref.shape[0] // 2
    total = jnp.sum(parts_ref[...].astype(F32), axis=0)
    out_ref[:half, :] = total[:, :HALF].astype(BF16)
    out_ref[half:, :] = flipped(total)[:, :HALF].astype(BF16)


def shape(dims, dtype):
    return jax.ShapeDtypeStruct(dims, dtype)


def shards(tokens, norm_gain, routes, gate_weights, expert_gate, expert_up, expert_down):
    rows, width = tokens.shape
    n_ep = lax.axis_size("ep")
    n_z = lax.axis_size("z")
    cap = rows // 2
    each = cap // 2
    slots = n_ep * cap
    mine = slots // 2
    part = width // 2
    w_gate, w_up, w_down = expert_gate[0], expert_up[0], expert_down[0]
    units = w_gate.shape[1]

    gain = norm_gain[None, :]
    picks = routes.T
    weights = gate_weights.T
    tables = jnp.asarray(slot_tables(each))
    hbm = pl.BlockSpec(memory_space=pltpu.HBM)
    vmem = pl.BlockSpec(memory_space=pltpu.VMEM)
    buffer, table = pl.pallas_call(
        dispatch_kernel,
        in_specs=[hbm] * 4,
        out_shape=(shape((mine, width), BF16), shape((2 * rows, slots), BF16)),
        out_specs=(hbm, vmem),
        scratch_shapes=[
            pltpu.VMEM(tokens.shape, tokens.dtype),
            pltpu.VMEM(picks.shape, picks.dtype),
            pltpu.VMEM(weights.shape, weights.dtype),
            pltpu.VMEM(tables.shape, tables.dtype),
            pltpu.VMEM((mine, width), BF16),
            pltpu.SemaphoreType.DMA((4,)),
            pltpu.SemaphoreType.DMA((4,)),
        ],
        compiler_params=params(8),
        name="dispatch",
    )(*in_hbm(tokens, picks, weights, tables))
    received = lax.all_to_all(
        buffer.reshape(n_ep, each, width),
        "ep",
        split_axis=0,
        concat_axis=0,
        tiled=True,
        axis_index_groups=[WAY_IN],
    ).reshape(mine, width)
    o_down = lax.ppermute(w_down, "c", SWAP)
    o_gate = lax.ppermute(w_gate, "c", SWAP)
    o_up = lax.ppermute(w_up, "c", SWAP)
    cut = width * 3 // 4
    head = pl.pallas_call(
        load_kernel,
        in_specs=[hbm],
        out_shape=shape((cut, units), BF16),
        scratch_shapes=[pltpu.SemaphoreType.DMA((1,))],
        compiler_params=params(8),
        name="load",
    )(*in_hbm(w_gate))
    hidden = pl.pallas_call(
        hidden_kernel,
        in_specs=[vmem] * 3 + [hbm] * 4,
        out_shape=shape((mine, 2 * units), BF16),
        scratch_shapes=[
            pltpu.VMEM((mine, width), BF16),
            pltpu.VMEM((width - cut, units), BF16),
            pltpu.VMEM(w_gate.shape, BF16),
            pltpu.VMEM(w_up.shape, BF16),
            pltpu.VMEM(w_up.shape, BF16),
            pltpu.SemaphoreType.DMA((4,)),
        ],
        compiler_params=params(8),
        name="hidden",
    )(received, gain, head, *in_hbm(w_gate, w_up, o_gate, o_up))
    outputs = pl.pallas_call(
        down_kernel,
        out_shape=shape((2 * n_ep, each, part), BF16),
        compiler_params=params(8),
        name="down",
    )(hidden, w_down, o_down)
    back = lax.all_to_all(
        outputs, ("ep", "c"), split_axis=0, concat_axis=0, tiled=True, axis_index_groups=[WAY_BACK]
    ).reshape(slots, part)
    packed = pl.pallas_call(
        combine_kernel,
        out_shape=shape((n_z, rows // 2, LANES), BF16),
        compiler_params=params(8),
        name="combine",
    )(table, back)
    parts = lax.all_to_all(packed, "z", split_axis=0, concat_axis=0, tiled=True, axis_index_groups=[ALONG_Z])
    return pl.pallas_call(
        total_kernel,
        out_shape=shape((rows, HALF), BF16),
        compiler_params=params(8),
        name="total",
    )(parts)


def solution(mesh):
    n_ep, n_tp = mesh.devices.shape
    chips = Mesh(np.asarray(mesh.devices).reshape(n_ep, n_tp // 2, 2), ("ep", "z", "c"))
    tp = ("z", "c")
    placed = (
        P("ep", None),
        P(),
        P("ep", None),
        P("ep", None),
        P("ep", None, tp),
        P("ep", None, tp),
        P("ep", tp, None),
    )
    return jax.shard_map(
        shards, mesh=chips, in_specs=placed, out_specs=P("ep", tp), check_vma=False
    )
```
